32 devices in a mesh: sp: 8 (over z, x), tp: 4 (over y, core).
Axes of the slice: x: 2, y: 2, z: 4, core: 2. Of those that a mesh axis runs over, the one named last changes fastest.
Arguments:
- pool_input: bfloat16 [4096, 512], P('sp', 'tp'), may hold values from -6 to 6
- documents: int32 [4096], P('sp'), may hold values from 0 to 1, never falling along the last dimension, each value on 1 to 3072 neighbouring positions
- group_weight: bfloat16 [4, 128, 128], P('tp'), may hold values from -0.5 to 0.5
- pool_scale: float32 [512], P('tp'), may hold values from 0.15 to 4.2, as said below
- pool_gain: float32 [512], P('tp'), may hold values from 0.1 to 1.9
- out_weight: bfloat16 [512, 2048], P('tp'), may hold values from -0.25 to 0.25
- residual: bfloat16 [4096, 2048], P(('sp', 'tp')), may hold values from -6 to 6
- routing: int32 [4096, 2], P(('sp', 'tp')), may hold values from 0 to 7, all different within a row; in each aligned block of 128 rows (0 to 127, 128 to 255, ...) at most 48 rows name the same one
- route_weights: float32 [4096, 2], P(('sp', 'tp')), may hold values from 0.2 to 0.9
- ffn_gain: float32 [2048], replicated, may hold values from 0.1 to 1.9
- expert_gate: bfloat16 [8, 2048, 3584], P('sp', None, 'tp'), may hold values from -0.125 to 0.125
- expert_up: bfloat16 [8, 2048, 3584], P('sp', None, 'tp'), may hold values from -0.125 to 0.125
- expert_down: bfloat16 [8, 3584, 2048], P('sp', 'tp'), may hold values from -0.09375 to 0.09375
Outputs:
- mixed: bfloat16 [4096, 2048], P(('sp', 'tp'))
The draws below stay inside these ranges and needn't reach their ends.
Inputs may be any that keep to these rules, and one draw needn't show every extreme that they name: `documents`: document numbers never fall along the sequence. `routing`: the two entries of a row differ. Among the rows of one device (128 rows in sp+tp order), no expert is named more than 48 times, a bound that some block reaches. `pool_scale`: Positive.
All inputs are finite; a program needn't handle non-finite values.
Results may differ from the reference program's by a relative error of at most 0.013.
Values may be sent and summed in bfloat16 or wider, within the bound.
A program may use at most 128 MiB of HBM per device.

```python
import math
import jax
import jax.numpy as jnp
import numpy as np
from jax import lax

D = 2048
FF = 3584
CH = 128
WINDOWS = 4
ROWS = 128
P_SIZE = 512
TOKENS = 4096
EXPERTS = 8
CAP = 48
DOCS = 2
DOC_MOST = 3072
N_TP = 4


def draw_pool_scale(key, part):
    levels = jnp.array([0.35, 0.7, 1.4, 2.8], jnp.float32)
    order_key, jitter_key = jax.random.split(key)
    ordering = jax.random.permutation(order_key, WINDOWS) % 4
    group_level = jnp.take(levels, ordering)
    jitter = 1.0 + 0.18 * jnp.clip(jax.random.normal(jitter_key, (WINDOWS, CH), jnp.float32), -2.5, 2.5)
    return (group_level[:, None] * jitter).reshape(WINDOWS * CH).astype(jnp.float32)


def block_scale(rng, shape, cuts, least, top_value):
    def one(position, parts):
        draws = jax.random.uniform(jax.random.fold_in(jax.random.fold_in(rng, 6), position), (parts,), jnp.float32, least / len(cuts), top_value / len(cuts))
        return jnp.repeat(jnp.exp(draws), shape[position] // parts).reshape((-1,) + (1,) * (len(shape) - position - 1))

    loudness = one(*cuts[0])
    for cut in cuts[1:]:
        loudness = loudness * one(*cut)
    return loudness


def split_up(amount, total, most, skew):
    loads = [(1 << 20) // math.isqrt(rank ** skew) + 1 for rank in range(2, amount + 1)]
    surplus, counts = total - most - (amount - 1), [1] * (amount - 1)
    while surplus > 0:
        movable = [i for i in range(amount - 1) if counts[i] < most]
        pool, budget = sum([loads[i] for i in movable]), surplus
        for i in movable:
            extra = min(most - counts[i], max(1, budget * loads[i] // pool), surplus)
            counts[i] = counts[i] + extra
            surplus = surplus - extra
    return np.array([most] + counts)


def uneven_parts(own_key, amount, total, bound, lean):
    if amount == 2:
        one = jax.random.randint(own_key, (), max(1, total - bound), min(bound, total - 1) + 1)
        return jnp.stack([one, total - one])
    sizes = jnp.asarray(split_up(amount, total, bound, lean), jnp.int32)
    couples = (amount - 1) // 2
    source_of, receiver = sizes[1:1 + 2 * couples:2], sizes[2:2 + 2 * couples:2]
    slack = jnp.minimum(source_of - 1, bound - receiver)
    passed = jax.random.randint(jax.random.fold_in(own_key, 1), (couples,), 0, 1 << 20) % (slack + 1)
    sizes = sizes.at[1:1 + 2 * couples:2].set(source_of - passed).at[2:2 + 2 * couples:2].set(receiver + passed)
    return sizes[jax.random.permutation(jax.random.fold_in(own_key, 2), amount)]


def assign_block(own_key, own, number, rows, amount, top, bound, skew):
    sequence = jax.random.permutation(own_key, amount)
    heavy_load, common = load_shares(amount, rows * top, bound, skew, True), load_shares(amount, rows * top, bound, skew, False)
    places = jnp.arange(amount)

    def named(tallies, turn):
        used = int((tallies > 0).sum())
        fixed = max(1, used // 4)
        moved = fixed + (places - fixed + turn * (used - fixed)) % max(1, amount - fixed)
        return jnp.zeros((amount,), jnp.int32).at[sequence[jnp.where(places < fixed, places, moved)]].set(jnp.asarray(tallies, jnp.int32))

    tallies = jnp.where(number % 4 == 0, named(heavy_load, number // 4), named(common, number - number // 4 - 1))
    mixed = jax.random.permutation(jax.random.fold_in(own, 3), amount)
    giver, taker = mixed[0:amount // 2 * 2:2], mixed[1:amount // 2 * 2:2]
    slack = jnp.minimum(tallies[giver] - 1, bound - tallies[taker]) // 2
    slack = jnp.where((giver == sequence[0]) | (taker == sequence[0]) | (tallies[taker] == 0), 0, jnp.maximum(slack, 0))
    moved = jax.random.randint(jax.random.fold_in(own, 4), (amount // 2,), 0, 1 << 20) % (slack + 1)
    tallies = tallies.at[giver].add(-moved).at[taker].add(moved)
    items = jnp.searchsorted(jnp.cumsum(tallies), jnp.arange(rows * top), side="right").astype(jnp.int32)
    table = items.reshape(top, rows).T
    table = table[jax.random.permutation(jax.random.fold_in(own, 1), rows)]
    turn = jax.random.randint(jax.random.fold_in(own, 2), (rows, 1), 0, top)
    return jnp.take_along_axis(table, (jnp.arange(top)[None, :] + turn) % top, axis=1)


def load_shares(amount, total, most, skew, full):
    portions = [(1 << 20) // math.isqrt(grade ** skew) + 1 for grade in range(1, amount + 1)]
    largest = most if full else min(most, max(-(-total // amount), total * portions[0] // sum(portions)))
    least = 1 if total - largest >= amount - 1 else 0
    holding, rest = [largest] + [least] * (amount - 1), total - largest - least * (amount - 1)
    while rest > 0:
        candidates = [i for i in range(1, amount) if holding[i] < largest] or [i for i in range(1, amount) if holding[i] < most]
        pool, remaining = sum([portions[i] for i in candidates]), rest
        for i in candidates:
            extra = min(most - holding[i], max(1, remaining * portions[i] // pool), rest)
            holding[i] = holding[i] + extra
            rest = rest - extra
    return np.array(holding)


def scatter_about(stream_key, extent, deviation, most, cuts=(), kind=jnp.bfloat16):
    level = block_scale(stream_key, extent, cuts, -0.22, 0.18) if cuts else 1.0
    values = jax.random.normal(stream_key, extent, jnp.float32) * deviation * level
    return jnp.minimum(jnp.maximum(values, -most), most).astype(kind)


def setup_inputs(seed: int = 0) -> dict:
    key_list = jax.random.split(jax.random.key(seed), 14)
    pool_input = scatter_about(key_list[0], (TOKENS, P_SIZE), 1.0, 6.0, ((0, 8), (1, 4)))
    documents = jnp.searchsorted(jnp.cumsum(uneven_parts(key_list[1], DOCS, TOKENS, DOC_MOST, 1)), jnp.arange(TOKENS), side="right").astype(jnp.int32)
    group_weight = scatter_about(key_list[2], (WINDOWS, CH, CH), CH ** -0.5, 0.5, ((0, 4),))
    pool_scale = draw_pool_scale(jax.random.fold_in(key_list[13], 71), 0)
    pool_gain = jnp.clip(1.0 + 0.18 * jax.random.normal(key_list[4], (P_SIZE,), jnp.float32), 0.1, 1.9)
    out_weight = scatter_about(key_list[5], (P_SIZE, D), P_SIZE ** -0.5, 0.25, ((0, 4),))
    residual = scatter_about(key_list[6], (TOKENS, D), 1.0, 6.0, ((0, 32),))
    routing_keys = jax.random.split(jax.random.fold_in(key_list[7], 1), TOKENS // ROWS)
    routing_turns = jax.random.permutation(jax.random.fold_in(key_list[7], 3), TOKENS // ROWS)
    routing = jax.vmap(lambda own, number: assign_block(jax.random.fold_in(key_list[7], 2), own, number, ROWS, EXPERTS, 2, CAP, 1))(routing_keys, routing_turns).reshape((TOKENS, 2))
    route_weights = jnp.clip(0.2 + 0.7 * jax.random.uniform(key_list[8], (TOKENS, 2), jnp.float32) ** block_scale(key_list[8], (TOKENS, 2), ((0, 32),), -0.2, 0.2), 0.2, 0.9)
    ffn_gain = jnp.clip(1.0 + 0.18 * jax.random.normal(key_list[9], (D,), jnp.float32), 0.1, 1.9)
    expert_gate = scatter_about(key_list[10], (EXPERTS, D, FF), D ** -0.5, 0.125, ((0, 8), (2, 4)))
    expert_up = scatter_about(key_list[11], (EXPERTS, D, FF), D ** -0.5, 0.125, ((0, 8), (2, 4)))
    expert_down = scatter_about(key_list[12], (EXPERTS, FF, D), FF ** -0.5, 0.09375, ((0, 8), (1, 4)))
    return {"pool_input": pool_input, "documents": documents, "group_weight": group_weight, "pool_scale": pool_scale, "pool_gain": pool_gain, "out_weight": out_weight, "residual": residual, "routing": routing, "route_weights": route_weights, "ffn_gain": ffn_gain, "expert_gate": expert_gate, "expert_up": expert_up, "expert_down": expert_down}


epsilon = 1e-06
window_lengths = (2, 4, 8, 16)

def round_trip(values):
    rounded = lax.optimization_barrier(values.astype(jnp.bfloat16))
    return rounded.astype(jnp.float32)

def window_means(extended, ext_docs, own_docs, length):
    reach = window_lengths[-1] - 1
    running = jnp.zeros((length, extended.shape[1]), jnp.float32)
    counted = jnp.zeros((length, 1), jnp.float32)
    results = []
    for offset in range(reach + 1):
        shifted = lax.slice_in_dim(extended, reach - offset, reach - offset + length, axis=0)
        earlier = lax.slice_in_dim(ext_docs, reach - offset, reach - offset + length, axis=0)
        inside = (earlier == own_docs).astype(jnp.float32)[:, None]
        running = running + inside * shifted
        counted = counted + inside
        if offset + 1 in window_lengths:
            results.append(running / counted)
    return results

def pool_branch(extended, ext_docs, own_docs, own_values, group_weight, pool_scale, first_group):
    stacked = jnp.stack(window_means(extended, ext_docs, own_docs, own_values.shape[0]))
    group_width = group_weight.shape[1]
    pieces = []
    for local_group in range(group_weight.shape[0]):
        chosen = lax.dynamic_index_in_dim(stacked, first_group + local_group, 0, keepdims=False)
        lower = local_group * group_width
        upper = lower + group_width
        difference = (chosen[:, lower:upper] - own_values[:, lower:upper]).astype(jnp.bfloat16)
        pieces.append(jnp.dot(difference, group_weight[local_group], preferred_element_type=jnp.float32))
    return jnp.concatenate(pieces, axis=1) * pool_scale

def norm_rows(middle, gain):
    widened = middle.astype(jnp.float32)
    inverse = lax.rsqrt(lax.optimization_barrier(jnp.mean(widened * widened, axis=1, keepdims=True)) + epsilon)
    return (widened * inverse * gain).astype(jnp.bfloat16)

def pick_slots(routes_block, capacity, expert_total):
    flat_picks = routes_block.reshape(-1)
    one_hot = (flat_picks[:, None] == jnp.arange(expert_total, dtype=jnp.int32)[None, :]).astype(jnp.int32)
    earlier_count = jnp.cumsum(one_hot, axis=0) - one_hot
    ranking = lax.optimization_barrier(jnp.sum(earlier_count * one_hot, axis=1))
    return (flat_picks * capacity + ranking).astype(jnp.int32)

def fill_slots(normed, slot_ids, total_slots):
    matches = (jnp.arange(total_slots, dtype=jnp.int32)[:, None] == slot_ids[None, :]).astype(jnp.int32)
    tokens_of = (jnp.arange(slot_ids.shape[0], dtype=jnp.int32) // 2)[None, :]
    owners = lax.optimization_barrier(jnp.sum(matches * tokens_of, axis=1)).astype(jnp.int32)
    filled = lax.optimization_barrier(jnp.sum(matches, axis=1)) > 0
    gathered = jnp.take(normed, owners, axis=0)
    return jnp.where(filled[:, None], gathered, jnp.zeros_like(gathered))

def combine_back(middle, returned, slot_ids, weights):
    picked = jnp.take(returned, slot_ids, axis=0).astype(jnp.float32)
    picked = picked.reshape(middle.shape[0], 2, middle.shape[1])
    summed = middle.astype(jnp.float32) + lax.optimization_barrier(jnp.sum(picked * weights[:, :, None], axis=1))
    return summed.astype(jnp.bfloat16)

def expert_hidden(inputs, gate_weight, up_weight):
    gate_sum = jnp.dot(inputs, gate_weight, preferred_element_type=jnp.float32)
    up_sum = jnp.dot(inputs, up_weight, preferred_element_type=jnp.float32)
    return (jax.nn.silu(gate_sum) * up_sum).astype(jnp.bfloat16)

def expert_output(inputs, gate_weight, up_weight, down_weight, pieces):
    hidden = expert_hidden(inputs, gate_weight, up_weight)
    piece_width = hidden.shape[1] // pieces
    summed = jnp.zeros((inputs.shape[0], down_weight.shape[1]), jnp.float32)
    for index_part in range(pieces):
        lower = index_part * piece_width
        upper = lower + piece_width
        summed = summed + round_trip(jnp.dot(hidden[:, lower:upper], down_weight[lower:upper], preferred_element_type=jnp.float32))
    return summed.astype(jnp.bfloat16)

def reference(pool_input, documents, group_weight, pool_scale, pool_gain, out_weight, residual, routing, route_weights, ffn_gain, expert_gate, expert_up, expert_down):
    reach = window_lengths[-1] - 1
    channels = pool_input.shape[1]
    width = residual.shape[1]
    own_values = pool_input.astype(jnp.float32)
    extended = jnp.concatenate([jnp.zeros((reach, channels), jnp.float32), own_values], axis=0)
    own_docs = (documents + 1).astype(jnp.int32)
    ext_docs = jnp.concatenate([jnp.zeros((reach,), jnp.int32), own_docs], axis=0)
    scaled = pool_branch(extended, ext_docs, own_docs, own_values, group_weight, pool_scale, 0)
    energy = lax.optimization_barrier(jnp.sum(scaled * scaled, axis=1, keepdims=True))
    gained = (scaled * pool_gain).astype(jnp.bfloat16)
    block_width = channels // N_TP
    summed = jnp.zeros((pool_input.shape[0], width), jnp.float32)
    for tp_part in range(N_TP):
        lower = tp_part * block_width
        upper = lower + block_width
        summed = summed + round_trip(jnp.dot(gained[:, lower:upper], out_weight[lower:upper], preferred_element_type=jnp.float32))
    projected = summed * lax.rsqrt(energy / channels + epsilon)
    middle = (residual.astype(jnp.float32) + projected).astype(jnp.bfloat16)
    normed = norm_rows(middle, ffn_gain)
    block_count = TOKENS // ROWS
    slot_ids = jax.vmap(lambda routes_block: pick_slots(routes_block, CAP, EXPERTS))(routing.reshape(block_count, ROWS, 2))
    buffers = jax.vmap(lambda normed_block, slots_block: fill_slots(normed_block, slots_block, EXPERTS * CAP))(normed.reshape(block_count, ROWS, width), slot_ids)
    by_expert = buffers.reshape(block_count, EXPERTS, CAP, width).transpose(1, 0, 2, 3).reshape(EXPERTS, block_count * CAP, width)

    def run_expert(operands):
        return expert_output(operands[0], operands[1], operands[2], operands[3], N_TP)
    outputs = lax.map(run_expert, (by_expert, expert_gate, expert_up, expert_down))
    returned = outputs.reshape(EXPERTS, block_count, CAP, width).transpose(1, 0, 2, 3).reshape(block_count, EXPERTS * CAP, width)
    mixed = jax.vmap(combine_back)(middle.reshape(block_count, ROWS, width), returned, slot_ids, route_weights.reshape(block_count, ROWS, 2))
    return mixed.reshape(TOKENS, width)
```

```python
import functools

import jax
import jax.numpy as jnp
from jax import lax
from jax.experimental import pallas as pl
from jax.experimental.pallas import tpu as pltpu
from jax.sharding import PartitionSpec as P

epsilon = 1e-06


def xor_index(value, other, size):
    result, bit = 0, 1
    while bit < size:
        result = result + ((value // bit + other // bit) % 2) * bit
        bit *= 2
    return result


def far_of(index, size):
    return size // 2 + index % 2 * (size // 4) + index // 2


def order_of(turn, size):
    half = size // 2
    late = turn // half
    return (1 - late) * far_of(turn % half, size) + late * (size - 1 - turn)


def sent_at(turn, me, size):
    half = size // 2
    far = turn // half
    swap = (me // 2 + me // 4 + 1) % 2
    step = (1 - far) * turn + far * (half + turn % half % 2 * (size // 4) + turn % half // 2)
    return xor_index(step, far * swap * (size // 4), size)


def remote(src, dst, sems, target):
    return pltpu.make_async_remote_copy(
        src_ref=src,
        dst_ref=dst,
        send_sem=sems[0],
        recv_sem=sems[1],
        device_id=target,
        device_id_type=pl.DeviceIdType.MESH,
    )


def turned(row, tokens):
    wide = jnp.broadcast_to(row, (tokens, row.shape[1]))
    return wide, wide.T


def moe_kernel(
    size,
    cap,
    pool,
    docs,
    group_weight,
    pool_scale,
    pool_gain,
    out_weight,
    residual,
    routing,
    route_weights,
    ffn_gain,
    gate_hbm,
    up_hbm,
    down_hbm,
    out,
    gate,
    up,
    down,
    hidden,
    sending,
    rows,
    part,
    from_core,
    from_y,
    back,
    acc,
    normed,
    slot_rows,
    slot_cols,
    weights,
    halo,
    halo_docs,
    gained,
    energy,
    far_gained,
    far_energy,
    wall,
    weight_sem,
    self_sem,
    d_s,
    d_r,
    y_s,
    y_r,
    c_s,
    c_r,
    p_s,
    p_r,
    q_s,
    q_r,
    t_s,
    t_r,
    halo_s,
    halo_r,
    wall_s,
    wall_r,
    gained_s,
    gained_r,
    energy_s,
    energy_r,
):
    me = lax.axis_index("sp")
    tp = lax.axis_index("tp")
    core, line = tp % 2, tp // 2
    place = core * 2 + line
    core_peer = {"tp": tp + 1 - 2 * core}
    line_peer = {"tp": (tp + 2) % 4}
    capp, width = sending.shape[1], sending.shape[2]
    tokens = residual.shape[0]

    loads = [
        pltpu.make_async_copy(src, dst, weight_sem.at[i])
        for i, (src, dst) in enumerate(((gate_hbm, gate), (up_hbm, up), (down_hbm, down)))
    ]
    for load in loads:
        load.start()

    row_ids = lax.broadcasted_iota(jnp.int32, (tokens, tokens), 0)
    col_ids = lax.broadcasted_iota(jnp.int32, (tokens, tokens), 1)

    def rank_slots():
        first_row, first_col = turned(routing[0:1, :].astype(jnp.float32), tokens)
        second_row, second_col = turned(routing[1:2, :].astype(jnp.float32), tokens)
        before, after = col_ids < row_ids, row_ids < col_ids

        def count(mask, axis):
            return jnp.sum(jnp.where(mask, 1.0, 0.0), axis=axis, keepdims=True)

        same_first, same_second = first_col == first_row, second_col == second_row
        slot_rows[0:1, :] = first_row[0:1, :] * cap + count(same_first & after, 0)
        slot_rows[1:2, :] = (
            second_row[0:1, :] * cap
            + count(first_col == second_row, 0)
            + count(same_second & after, 0)
        )
        slot_cols[0] = first_col * cap + count(same_first & before, 1)
        slot_cols[1] = (
            second_col * cap + count(second_col == first_row, 1) + count(same_second & before, 1)
        )
        weights[0] = turned(route_weights[0:1, :], tokens)[1]
        weights[1] = turned(route_weights[1:2, :], tokens)[1]

    def prefix():
        total = docs.shape[1]
        near = tp + 2 - 4 * line
        behind = [
            remote(
                pool.at[pl.ds(total - tokens, tokens)],
                halo,
                (halo_s.at[0], halo_r.at[0]),
                {"sp": (me + 1) % size},
            ),
            remote(
                docs.at[:, pl.ds(total - tokens, tokens)],
                halo_docs,
                (halo_s.at[1], halo_r.at[1]),
                {"sp": (me + 1) % size},
            ),
        ]

        @pl.when(me < size - 1)
        def _():
            for copy in behind:
                copy.start()

        side = me % 2
        piece = out_weight.shape[0] // 8

        def strip(first, count):
            return pl.ds(pl.multiple_of(first * piece, piece), count * piece)

        def moved(src, place, index, target):
            return remote(src, place, (wall_s.at[index], wall_r.at[index]), target)

        def handed_on(rows_of, index, target):
            block = wall.at[near, rows_of]
            return moved(block, block, index, target)

        mine = [strip(5 * side + i, 1) for i in range(3)]
        middle_rows = strip(3, 2)
        to_line = [
            moved(out_weight.at[rows_of], wall.at[tp, rows_of], i, line_peer)
            for i, rows_of in enumerate([*mine, middle_rows])
        ]
        to_side = [
            handed_on(rows_of, 4 + i, {"sp": me + 1 - 2 * side}) for i, rows_of in enumerate(mine)
        ]
        from_side = [
            handed_on(strip(5 * (1 - side) + i, 1), 4 + i, {"sp": me + 1 - 2 * side})
            for i in range(3)
        ]
        to_core = moved(out_weight, wall.at[tp], 7, core_peer)
        relayed = [
            handed_on(rows_of, 8 + i, core_peer)
            for i, rows_of in enumerate(
                [strip(5 * side, 3), strip(5 * (1 - side), 3), middle_rows]
            )
        ]
        for copy in to_line[:3]:
            copy.start()
        to_core.start()

        reach = 2 * (1 + core) * (1 + 3 * line)
        def pooled(index):
            here = pl.ds(index * tokens, tokens)
            before = pl.ds((index - 1) * tokens, tokens)
            own = pool[here, :]
            earlier = pool[before, :] if index else halo[...]
            doc_row, doc_col = turned(docs[:, here].astype(jnp.float32), tokens)
            old_row = (docs[:, before] if index else halo_docs[...]).astype(jnp.float32)
            inside = (doc_row == doc_col) & (col_ids <= row_ids) & (col_ids > row_ids - reach)
            outside = (old_row == doc_col) & (col_ids - tokens > row_ids - reach)
            inside = jnp.where(inside, 1.0, 0.0)
            outside = jnp.where(outside, 1.0, 0.0)
            counted = jnp.sum(inside + outside, axis=1, keepdims=True)
            running = jnp.dot(
                inside.astype(jnp.bfloat16), own, preferred_element_type=jnp.float32
            ) + jnp.dot(outside.astype(jnp.bfloat16), earlier, preferred_element_type=jnp.float32)
            difference = (running / counted - own.astype(jnp.float32)).astype(jnp.bfloat16)
            scaled = (
                jnp.dot(difference, group_weight[0], preferred_element_type=jnp.float32)
                * pool_scale[...]
            )
            gained[index] = (scaled * pool_gain[...]).astype(jnp.bfloat16)
            squares = jnp.sum((scaled * scaled).T, axis=0, keepdims=True)
            energy[index] = jnp.broadcast_to(squares, energy.shape[1:])

        for index in range(1, total // tokens):
            pooled(index)

        @pl.when(me == 0)
        def _():
            halo[...] = jnp.zeros_like(halo)
            halo_docs[...] = jnp.full_like(halo_docs, -1)

        @pl.when(me > 0)
        def _():
            for copy in behind:
                copy.wait_recv()

        pooled(0)

        def trade(away):
            to = (tp + away) % 4
            return (
                remote(
                    gained.at[to],
                    far_gained.at[away],
                    (gained_s.at[away], gained_r.at[away]),
                    {"tp": to},
                ),
                remote(
                    energy.at[to],
                    far_energy.at[away],
                    (energy_s.at[away], energy_r.at[away]),
                    {"tp": to},
                ),
            )

        for away in range(1, 4):
            for copy in trade(away):
                copy.start()
        to_line[3].start()
        acc[...] = jnp.dot(gained[tp], out_weight[...], preferred_element_type=jnp.float32)
        for arrived, onward in zip(to_line[:3], to_side):
            arrived.wait_recv()
            onward.start()
        relayed[0].start()
        squared = energy[tp]
        for away in range(1, 4):
            for copy in trade(away):
                copy.wait_recv()
            squared = squared + far_energy[away]

        def project(source):
            away = (tp + 4 - source) % 4
            acc[...] += jnp.dot(
                far_gained[away], wall[source], preferred_element_type=jnp.float32
            )

        to_core.wait_recv()
        project(tp + 1 - 2 * core)
        to_line[3].wait_recv()
        relayed[2].start()
        for copy in from_side:
            copy.wait_recv()
        relayed[1].start()
        project(near)
        for copy in relayed:
            copy.wait_recv()
        project(near + 1 - 2 * core)
        energy_col = turned(squared[0:1, :], tokens)[1][:, 0:1]
        scale = lax.rsqrt(energy_col / (4 * pool.shape[1]) + epsilon)
        middle = (residual[...].astype(jnp.float32) + acc[...] * scale).astype(jnp.bfloat16)
        middle = middle.astype(jnp.float32)
        acc[...] = middle
        inverse = lax.rsqrt(jnp.mean(middle * middle, axis=1, keepdims=True) + epsilon)
        normed[...] = (middle * inverse * ffn_gain[...]).astype(jnp.bfloat16)

        @pl.when(me < size - 1)
        def _():
            for copy in behind:
                copy.wait_send()

        for copy in (*to_line, *to_side, to_core, *relayed):
            copy.wait_send()
        for away in range(1, 4):
            for copy in trade(away):
                copy.wait_send()

    barrier = pltpu.get_barrier_semaphore()

    def greet(step, carry):
        peer = xor_index(me, step, size)
        pl.semaphore_signal(
            barrier, inc=1, device_id={"sp": peer}, device_id_type=pl.DeviceIdType.MESH
        )
        return carry

    lax.fori_loop(1, size, greet, 0)
    for away in range(1, 4):
        pl.semaphore_signal(
            barrier,
            inc=1,
            device_id={"tp": (tp + away) % 4},
            device_id_type=pl.DeviceIdType.MESH,
        )
    rank_slots()
    pl.semaphore_wait(barrier, size + 2)
    prefix()

    def peer_of(step):
        return xor_index(me, step, size)

    def dispatch(step):
        return remote(
            sending.at[step], rows.at[step, place], (d_s.at[step], d_r.at[step]), {"sp": peer_of(step)}
        )

    def across_line(step):
        return remote(
            rows.at[step, place], rows.at[step, place], (y_s.at[step], y_r.at[step]), line_peer
        )

    def across_core(step):
        block = rows.at[step, pl.ds(2 * core, 2)]
        return remote(block, block, (c_s.at[step], c_r.at[step]), core_peer)

    def core_sum(step):
        return remote(
            part.at[step, pl.ds(2 * (1 - core), 2)],
            from_core.at[step],
            (p_s.at[step], p_r.at[step]),
            core_peer,
        )

    def line_sum(step):
        return remote(
            part.at[step, 2 * core + 1 - line],
            from_y.at[step],
            (q_s.at[step], q_r.at[step]),
            line_peer,
        )

    def give_back(step):
        return remote(
            part.at[step, place], back.at[step], (t_s.at[step], t_r.at[step]), {"sp": peer_of(step)}
        )

    def filled(step):
        first = peer_of(step) * cap
        position = lax.broadcasted_iota(jnp.int32, (capp, tokens), 0)
        wanted = jnp.where(position < cap, position + first, -1).astype(jnp.float32)
        match = (wanted == slot_rows[0:1, :]) | (wanted == slot_rows[1:2, :])
        return jnp.dot(
            match.astype(jnp.float32).astype(jnp.bfloat16),
            normed[...],
            preferred_element_type=jnp.float32,
        ).astype(jnp.bfloat16)

    def send_rows(turn, carry):
        step = sent_at(turn, me, size)
        sending[step] = filled(step)
        dispatch(step).start()
        return carry

    sending[0] = filled(0)
    own = pltpu.make_async_copy(sending.at[0], rows.at[0, place], self_sem.at[0])
    own.start()
    lax.fori_loop(1, size, send_rows, 0)
    own.wait()
    across_line(0).start()
    for load in loads:
        load.wait()

    def gate_up(step):
        block = rows[step]
        if capp % 16:
            block = block.astype(jnp.float32).reshape(4 * capp, width).astype(jnp.bfloat16)
        else:
            block = block.reshape(4 * capp, width)
        gate_sum = jnp.dot(block, gate[...], preferred_element_type=jnp.float32)
        up_sum = jnp.dot(block, up[...], preferred_element_type=jnp.float32)
        hidden[...] = (gate_sum / (1.0 + jnp.exp(-gate_sum)) * up_sum).astype(jnp.bfloat16)

    def downward(step):
        result = jnp.dot(hidden[...], down[...], preferred_element_type=jnp.float32)
        part[step] = result.reshape(4, capp, width).astype(jnp.bfloat16)

    half = size // 2

    def arrive(step):
        dispatch(step).wait_recv()
        across_line(step).start()

    def share(step):
        across_line(step).wait_recv()
        across_core(step).start()

    def reduce_core(step):
        core_sum(step).wait_recv()
        other = 2 * core + 1 - line
        total = part[step, other].astype(jnp.float32) + from_core[step, 1 - line].astype(
            jnp.float32
        )
        part[step, other] = total.astype(jnp.bfloat16)
        line_sum(step).start()

    def reduce_line(step):
        line_sum(step).wait_recv()
        total = (
            part[step, place].astype(jnp.float32)
            + from_core[step, line].astype(jnp.float32)
            + from_y[step].astype(jnp.float32)
        )
        part[step, place] = total.astype(jnp.bfloat16)

        @pl.when(step >= 1)
        def _():
            give_back(step).start()

    def body(turn, carry):
        step = order_of(turn, size)
        across_core(step).wait_recv()
        gate_up(step)

        @pl.when(turn >= half + 1)
        def _():
            reduce_core(order_of(turn - 1, size))

        downward(step)
        core_sum(step).start()

        @pl.when(turn + 2 < half)
        def _():
            arrive(far_of(turn + 2, size))

        @pl.when(turn < half)
        def _():
            reduce_core(step)

        @pl.when(turn + 1 < half)
        def _():
            share(far_of(turn + 1, size))

        @pl.when((turn >= 1) & (turn < half))
        def _():
            reduce_line(order_of(turn - 1, size))

        @pl.when(turn >= half + 1)
        def _():
            reduce_line(order_of(turn - 2, size))

        return carry

    def near(step, carry):
        share(step)
        return carry

    arrive(1)
    share(0)

    def early(step, carry):
        arrive(step)
        return carry

    lax.fori_loop(2, half, early, 0)
    arrive(far_of(0, size))
    lax.fori_loop(1, half, near, 0)
    arrive(far_of(1, size))
    share(far_of(0, size))
    lax.fori_loop(0, size, body, 0)
    reduce_core(0)
    reduce_line(1)
    reduce_line(0)

    def returned(step, carry):
        give_back(step).wait_recv()
        return carry

    back[0] = part[0, place]
    position = lax.broadcasted_iota(jnp.int32, (tokens, size * capp), 1)
    block, offset = position // capp, position % capp
    expert_of = xor_index(block, me, size)
    wanted = jnp.where(offset < cap, expert_of * cap + offset, -1).astype(jnp.float32)
    chosen = jnp.where(wanted == slot_cols[0, :, 0:1], weights[0, :, 0:1], 0.0) + jnp.where(
        wanted == slot_cols[1, :, 0:1], weights[1, :, 0:1], 0.0
    )
    high = chosen.astype(jnp.bfloat16)
    low = (chosen - high.astype(jnp.float32)).astype(jnp.bfloat16)
    lax.fori_loop(1, size, returned, 0)
    values = back[...]
    if capp % 16:
        values = values.astype(jnp.float32).reshape(size * capp, width).astype(jnp.bfloat16)
    else:
        values = values.reshape(size * capp, width)
    acc[...] += jnp.dot(high, values, preferred_element_type=jnp.float32) + jnp.dot(
        low, values, preferred_element_type=jnp.float32
    )
    out[...] = acc[...].astype(jnp.bfloat16)

    def finish(step, carry):
        @pl.when(step >= 1)
        def _():
            dispatch(step).wait_send()
            give_back(step).wait_send()

        across_line(step).wait_send()
        across_core(step).wait_send()
        core_sum(step).wait_send()
        line_sum(step).wait_send()
        return carry

    lax.fori_loop(0, size, finish, 0)


def on_device(
    pool_input,
    documents,
    group_weight,
    pool_scale,
    pool_gain,
    out_weight,
    residual,
    routing,
    route_weights,
    ffn_gain,
    expert_gate,
    expert_up,
    expert_down,
):
    size = lax.axis_size("sp")
    tokens, width = residual.shape
    channels = pool_input.shape[1]
    gate, up, down = expert_gate[0], expert_up[0], expert_down[0]
    capacity = (3 * tokens + size - 1) // size
    padded = (capacity + 7) // 8 * 8
    vmem = pl.BlockSpec(memory_space=pltpu.VMEM)
    hbm = pl.BlockSpec(memory_space=pl.ANY)
    block = (padded, width)
    return pl.pallas_call(
        functools.partial(moe_kernel, size, capacity),
        out_shape=jax.ShapeDtypeStruct((tokens, width), jnp.bfloat16),
        in_specs=[vmem] * 10 + [hbm] * 3,
        out_specs=vmem,
        scratch_shapes=[
            pltpu.VMEM(gate.shape, jnp.bfloat16),
            pltpu.VMEM(up.shape, jnp.bfloat16),
            pltpu.VMEM(down.shape, jnp.bfloat16),
            pltpu.VMEM((4 * padded, down.shape[0]), jnp.bfloat16),
            pltpu.VMEM((size,) + block, jnp.bfloat16),
            pltpu.VMEM((size, 4) + block, jnp.bfloat16),
            pltpu.VMEM((size, 4) + block, jnp.bfloat16),
            pltpu.VMEM((size, 2) + block, jnp.bfloat16),
            pltpu.VMEM((size,) + block, jnp.bfloat16),
            pltpu.VMEM((size,) + block, jnp.bfloat16),
            pltpu.VMEM((tokens, width), jnp.float32),
            pltpu.VMEM((tokens, width), jnp.bfloat16),
            pltpu.VMEM((2, tokens), jnp.float32),
            pltpu.VMEM((2, tokens, tokens), jnp.float32),
            pltpu.VMEM((2, tokens, tokens), jnp.float32),
            pltpu.VMEM((tokens, channels), jnp.bfloat16),
            pltpu.VMEM((1, tokens), jnp.int32),
            pltpu.VMEM((4, tokens, channels), jnp.bfloat16),
            pltpu.VMEM((4, 8, tokens), jnp.float32),
            pltpu.VMEM((4, tokens, channels), jnp.bfloat16),
            pltpu.VMEM((4, 8, tokens), jnp.float32),
            pltpu.VMEM((4, channels, width), jnp.bfloat16),
            pltpu.SemaphoreType.DMA((3,)),
            pltpu.SemaphoreType.DMA((1,)),
        ]
        + [pltpu.SemaphoreType.DMA((size,))] * 12
        + [pltpu.SemaphoreType.DMA((2,))] * 2
        + [pltpu.SemaphoreType.DMA((11,))] * 2
        + [pltpu.SemaphoreType.DMA((4,))] * 4,
        compiler_params=pltpu.CompilerParams(
            collective_id=0, has_side_effects=True, vmem_limit_bytes=62 * 1024 * 1024
        ),
    )(
        pool_input,
        documents.reshape(1, -1),
        group_weight,
        pool_scale.reshape(1, -1),
        pool_gain.reshape(1, -1),
        out_weight,
        residual,
        routing.T,
        route_weights.T,
        ffn_gain.reshape(1, -1),
        gate,
        up,
        down,
    )


def solution(mesh):
    return jax.shard_map(
        on_device,
        mesh=mesh,
        in_specs=(
            P("sp", "tp"),
            P("sp"),
            P("tp", None, None),
            P("tp"),
            P("tp"),
            P("tp", None),
            P(("sp", "tp"), None),
            P(("sp", "tp"), None),
            P(("sp", "tp"), None),
            P(),
            P("sp", None, "tp"),
            P("sp", None, "tp"),
            P("sp", "tp", None),
        ),
        out_specs=P(("sp", "tp"), None),
        check_vma=False,
    )
```

```python
import functools

import jax
import jax.numpy as jnp
from jax import lax
from jax.experimental import pallas as pl
from jax.experimental.pallas import tpu as pltpu
from jax.sharding import PartitionSpec as P

epsilon = 1e-06


def xor_index(value, other, size):
    result, bit = 0, 1
    while bit < size:
        result = result + ((value // bit + other // bit) % 2) * bit
        bit *= 2
    return result


def far_of(index, size):
    return size // 2 + index % 2 * (size // 4) + index // 2


def order_of(turn, size):
    half = size // 2
    early = (size - turn) // (half + 2)
    last = turn // half * ((size - 1 - turn) // (half - 1))
    far = early + last
    return far * far_of((turn - last) % half, size) + (1 - far) * (size - 1 - turn - (size - turn) // (half + 1))


def sent_at(turn, size):
    odd, last = turn % 2, turn // (size - 2)
    far = odd + last
    return far * far_of(turn // 2, size) + (1 - far) * (turn // 2 + 1)


def remote(src, dst, sems, target):
    return pltpu.make_async_remote_copy(
        src_ref=src,
        dst_ref=dst,
        send_sem=sems[0],
        recv_sem=sems[1],
        device_id=target,
        device_id_type=pl.DeviceIdType.MESH,
    )


def turned(row, tokens):
    wide = jnp.broadcast_to(row, (tokens, row.shape[1]))
    return wide, wide.T


def moe_kernel(
    size,
    cap,
    pool,
    docs,
    group_weight,
    pool_scale,
    pool_gain,
    out_weight,
    residual,
    routing,
    route_weights,
    ffn_gain,
    gate_hbm,
    up_hbm,
    down_hbm,
    out,
    gate,
    up,
    down,
    hidden,
    sending,
    rows,
    part,
    from_core,
    from_y,
    back,
    acc,
    normed,
    slot_rows,
    slot_cols,
    weights,
    halo,
    halo_docs,
    gained,
    energy,
    far_gained,
    far_energy,
    wall,
    weight_sem,
    d_s,
    d_r,
    y_s,
    y_r,
    c_s,
    c_r,
    p_s,
    p_r,
    q_s,
    q_r,
    t_s,
    t_r,
    halo_s,
    halo_r,
    wall_s,
    wall_r,
    gained_s,
    gained_r,
    energy_s,
    energy_r,
):
    me = lax.axis_index("sp")
    tp = lax.axis_index("tp")
    core, line = tp % 2, tp // 2
    place = core * 2 + line
    core_peer = {"tp": tp + 1 - 2 * core}
    line_peer = {"tp": (tp + 2) % 4}
    capp, width = sending.shape[1], sending.shape[2]
    tokens = residual.shape[0]

    loads = [
        pltpu.make_async_copy(src, dst, weight_sem.at[i])
        for i, (src, dst) in enumerate(((gate_hbm, gate), (up_hbm, up), (down_hbm, down)))
    ]
    for load in loads:
        load.start()

    row_ids = lax.broadcasted_iota(jnp.int32, (tokens, tokens), 0)
    col_ids = lax.broadcasted_iota(jnp.int32, (tokens, tokens), 1)

    def rank_slots():
        first_row, first_col = turned(routing[0:1, :].astype(jnp.float32), tokens)
        second_row, second_col = turned(routing[1:2, :].astype(jnp.float32), tokens)
        before, after = col_ids < row_ids, row_ids < col_ids

        def count(mask, axis):
            return jnp.sum(jnp.where(mask, 1.0, 0.0), axis=axis, keepdims=True)

        same_first, same_second = first_col == first_row, second_col == second_row
        slot_rows[0:1, :] = first_row[0:1, :] * cap + count(same_first & after, 0)
        slot_rows[1:2, :] = (
            second_row[0:1, :] * cap
            + count(first_col == second_row, 0)
            + count(same_second & after, 0)
        )
        slot_cols[0] = first_col * cap + count(same_first & before, 1)
        slot_cols[1] = (
            second_col * cap + count(second_col == first_row, 1) + count(same_second & before, 1)
        )
        weights[0] = turned(route_weights[0:1, :], tokens)[1]
        weights[1] = turned(route_weights[1:2, :], tokens)[1]

    def prefix():
        total = docs.shape[1]
        near = tp + 2 - 4 * line
        behind = [
            remote(
                pool.at[pl.ds(total - tokens, tokens)],
                halo,
                (halo_s.at[0], halo_r.at[0]),
                {"sp": (me + 1) % size},
            ),
            remote(
                docs.at[:, pl.ds(total - tokens, tokens)],
                halo_docs,
                (halo_s.at[1], halo_r.at[1]),
                {"sp": (me + 1) % size},
            ),
        ]

        @pl.when(me < size - 1)
        def _():
            for copy in behind:
                copy.start()

        side = me % 2
        piece = out_weight.shape[0] // 8

        def strip(first, count):
            return pl.ds(pl.multiple_of(first * piece, piece), count * piece)

        def moved(src, place, index, target):
            return remote(src, place, (wall_s.at[index], wall_r.at[index]), target)

        def handed_on(rows_of, index, target):
            block = wall.at[near, rows_of]
            return moved(block, block, index, target)

        mine = [strip(5 * side + i, 1) for i in range(3)]
        middle_rows = strip(3, 2)
        to_line = [
            moved(out_weight.at[rows_of], wall.at[tp, rows_of], i, line_peer)
            for i, rows_of in enumerate([*mine, middle_rows])
        ]
        to_side = [
            handed_on(rows_of, 4 + i, {"sp": me + 1 - 2 * side}) for i, rows_of in enumerate(mine)
        ]
        from_side = [
            handed_on(strip(5 * (1 - side) + i, 1), 4 + i, {"sp": me + 1 - 2 * side})
            for i in range(3)
        ]
        to_core = moved(out_weight, wall.at[tp], 7, core_peer)
        relayed = [
            handed_on(rows_of, 8 + i, core_peer)
            for i, rows_of in enumerate(
                [strip(5 * side, 3), strip(5 * (1 - side), 3), middle_rows]
            )
        ]
        for copy in to_line[:3]:
            copy.start()
        to_core.start()

        reach = 2 * (1 + core) * (1 + 3 * line)
        def pooled(index):
            here = pl.ds(index * tokens, tokens)
            before = pl.ds((index - 1) * tokens, tokens)
            own = pool[here, :]
            earlier = pool[before, :] if index else halo[...]
            doc_row, doc_col = turned(docs[:, here].astype(jnp.float32), tokens)
            old_row = (docs[:, before] if index else halo_docs[...]).astype(jnp.float32)
            inside = (doc_row == doc_col) & (col_ids <= row_ids) & (col_ids > row_ids - reach)
            outside = (old_row == doc_col) & (col_ids - tokens > row_ids - reach)
            inside = jnp.where(inside, 1.0, 0.0)
            outside = jnp.where(outside, 1.0, 0.0)
            counted = jnp.sum(inside + outside, axis=1, keepdims=True)
            running = jnp.dot(
                inside.astype(jnp.bfloat16), own, preferred_element_type=jnp.float32
            ) + jnp.dot(outside.astype(jnp.bfloat16), earlier, preferred_element_type=jnp.float32)
            difference = (running / counted - own.astype(jnp.float32)).astype(jnp.bfloat16)
            scaled = (
                jnp.dot(difference, group_weight[0], preferred_element_type=jnp.float32)
                * pool_scale[...]
            )
            gained[index] = (scaled * pool_gain[...]).astype(jnp.bfloat16)
            squares = jnp.sum((scaled * scaled).T, axis=0, keepdims=True)
            energy[index] = jnp.broadcast_to(squares, energy.shape[1:])

        for index in range(1, total // tokens):
            pooled(index)

        @pl.when(me == 0)
        def _():
            halo[...] = jnp.zeros_like(halo)
            halo_docs[...] = jnp.full_like(halo_docs, -1)

        @pl.when(me > 0)
        def _():
            for copy in behind:
                copy.wait_recv()

        pooled(0)

        def trade(away):
            to = (tp + away) % 4
            return (
                remote(
                    gained.at[to],
                    far_gained.at[away],
                    (gained_s.at[away], gained_r.at[away]),
                    {"tp": to},
                ),
                remote(
                    energy.at[to],
                    far_energy.at[away],
                    (energy_s.at[away], energy_r.at[away]),
                    {"tp": to},
                ),
            )

        for away in range(1, 4):
            for copy in trade(away):
                copy.start()
        to_line[3].start()
        acc[...] = jnp.dot(gained[tp], out_weight[...], preferred_element_type=jnp.float32)
        for arrived, onward in zip(to_line[:3], to_side):
            arrived.wait_recv()
            onward.start()
        relayed[0].start()
        squared = energy[tp]
        for away in range(1, 4):
            for copy in trade(away):
                copy.wait_recv()
            squared = squared + far_energy[away]

        def project(source):
            away = (tp + 4 - source) % 4
            acc[...] += jnp.dot(
                far_gained[away], wall[source], preferred_element_type=jnp.float32
            )

        to_core.wait_recv()
        project(tp + 1 - 2 * core)
        to_line[3].wait_recv()
        relayed[2].start()
        for copy in from_side:
            copy.wait_recv()
        relayed[1].start()
        project(near)
        for copy in relayed:
            copy.wait_recv()
        project(near + 1 - 2 * core)
        energy_col = turned(squared[0:1, :], tokens)[1][:, 0:1]
        scale = lax.rsqrt(energy_col / (4 * pool.shape[1]) + epsilon)
        middle = (residual[...].astype(jnp.float32) + acc[...] * scale).astype(jnp.bfloat16)
        middle = middle.astype(jnp.float32)
        acc[...] = middle
        inverse = lax.rsqrt(jnp.mean(middle * middle, axis=1, keepdims=True) + epsilon)
        normed[...] = (middle * inverse * ffn_gain[...]).astype(jnp.bfloat16)

        @pl.when(me < size - 1)
        def _():
            for copy in behind:
                copy.wait_send()

        for copy in (*to_line, *to_side, to_core, *relayed):
            copy.wait_send()
        for away in range(1, 4):
            for copy in trade(away):
                copy.wait_send()

    barrier = pltpu.get_barrier_semaphore()

    def greet(step, carry):
        peer = xor_index(me, step, size)
        pl.semaphore_signal(
            barrier, inc=1, device_id={"sp": peer}, device_id_type=pl.DeviceIdType.MESH
        )
        return carry

    lax.fori_loop(1, size, greet, 0)
    for away in range(1, 4):
        pl.semaphore_signal(
            barrier,
            inc=1,
            device_id={"tp": (tp + away) % 4},
            device_id_type=pl.DeviceIdType.MESH,
        )
    rank_slots()
    pl.semaphore_wait(barrier, size + 2)
    prefix()

    def peer_of(step):
        return xor_index(me, step, size)

    def dispatch(step):
        return remote(
            sending.at[step], rows.at[step, place], (d_s.at[step], d_r.at[step]), {"sp": peer_of(step)}
        )

    def across_line(step):
        return remote(
            rows.at[step, place], rows.at[step, place], (y_s.at[step], y_r.at[step]), line_peer
        )

    def across_core(step):
        block = rows.at[step, pl.ds(2 * core, 2)]
        return remote(block, block, (c_s.at[step], c_r.at[step]), core_peer)

    def core_sum(step):
        return remote(
            part.at[step, pl.ds(2 * (1 - core), 2)],
            from_core.at[step],
            (p_s.at[step], p_r.at[step]),
            core_peer,
        )

    def line_sum(step):
        return remote(
            part.at[step, 2 * core + 1 - line],
            from_y.at[step],
            (q_s.at[step], q_r.at[step]),
            line_peer,
        )

    def give_back(step):
        return remote(
            part.at[step, place], back.at[step], (t_s.at[step], t_r.at[step]), {"sp": peer_of(step)}
        )

    def filled(step):
        first = peer_of(step) * cap
        position = lax.broadcasted_iota(jnp.int32, (capp, tokens), 0)
        wanted = jnp.where(position < cap, position + first, -1).astype(jnp.float32)
        match = (wanted == slot_rows[0:1, :]) | (wanted == slot_rows[1:2, :])
        return jnp.dot(
            match.astype(jnp.float32).astype(jnp.bfloat16),
            normed[...],
            preferred_element_type=jnp.float32,
        ).astype(jnp.bfloat16)

    def send_rows(turn, carry):
        step = sent_at(turn, size)
        sending[step] = filled(step)
        dispatch(step).start()
        return carry

    rows[0, place] = filled(0)
    across_line(0).start()
    lax.fori_loop(0, size - 1, send_rows, 0)
    for load in loads:
        load.wait()

    def gate_up(step):
        block = rows[step]
        if capp % 16:
            block = block.astype(jnp.float32).reshape(4 * capp, width).astype(jnp.bfloat16)
        else:
            block = block.reshape(4 * capp, width)
        gate_sum = jnp.dot(block, gate[...], preferred_element_type=jnp.float32)
        up_sum = jnp.dot(block, up[...], preferred_element_type=jnp.float32)
        hidden[...] = (gate_sum / (1.0 + jnp.exp(-gate_sum)) * up_sum).astype(jnp.bfloat16)

    def downward(step):
        result = jnp.dot(hidden[...], down[...], preferred_element_type=jnp.float32)
        part[step] = result.reshape(4, capp, width).astype(jnp.bfloat16)

    half = size // 2

    def arrive(step):
        dispatch(step).wait_recv()
        across_line(step).start()

    def share(step):
        across_line(step).wait_recv()
        across_core(step).start()

    def reduce_core(step):
        core_sum(step).wait_recv()
        other = 2 * core + 1 - line
        total = part[step, other].astype(jnp.float32) + from_core[step, 1 - line].astype(
            jnp.float32
        )
        part[step, other] = total.astype(jnp.bfloat16)
        line_sum(step).start()

    def reduce_line(step):
        line_sum(step).wait_recv()
        total = (
            part[step, place].astype(jnp.float32)
            + from_core[step, line].astype(jnp.float32)
            + from_y[step].astype(jnp.float32)
        )
        part[step, place] = total.astype(jnp.bfloat16)

        @pl.when(step >= 1)
        def _():
            give_back(step).start()

    def body(turn, carry):
        step = order_of(turn, size)

        @pl.when(turn + 1 < half)
        def _():
            arrive(far_of(turn + 1, size))

        across_core(step).wait_recv()
        gate_up(step)

        @pl.when(turn == half - 1)
        def _():
            share(far_of(turn, size))

        @pl.when((turn >= half) & (turn != half + 1))
        def _():
            reduce_core(order_of(turn - 1, size))

        @pl.when(turn >= half)
        def _():
            reduce_line(order_of(turn - 2, size))

        downward(step)
        core_sum(step).start()

        @pl.when((turn + 1 < half) | (turn == half))
        def _():
            reduce_core(step)

        @pl.when(turn + 3 < half)
        def _():
            arrive(turn + 3)

        @pl.when((turn >= 1) & (turn + 1 < half))
        def _():
            reduce_line(order_of(turn - 1, size))
            share(turn + 1)

        @pl.when(turn + 2 < half)
        def _():
            share(far_of(turn + 1, size))

        return carry

    arrive(1)
    arrive(far_of(0, size))
    share(0)
    share(1)
    arrive(2)
    share(far_of(0, size))
    lax.fori_loop(0, size, body, 0)
    reduce_core(0)
    reduce_line(1)
    reduce_line(0)

    def returned(step, carry):
        give_back(step).wait_recv()
        return carry

    back[0] = part[0, place]
    position = lax.broadcasted_iota(jnp.int32, (tokens, size * capp), 1)
    block, offset = position // capp, position % capp
    expert_of = xor_index(block, me, size)
    wanted = jnp.where(offset < cap, expert_of * cap + offset, -1).astype(jnp.float32)
    chosen = jnp.where(wanted == slot_cols[0, :, 0:1], weights[0, :, 0:1], 0.0) + jnp.where(
        wanted == slot_cols[1, :, 0:1], weights[1, :, 0:1], 0.0
    )
    high = chosen.astype(jnp.bfloat16)
    low = (chosen - high.astype(jnp.float32)).astype(jnp.bfloat16)
    lax.fori_loop(1, size, returned, 0)
    values = back[...]
    if capp % 16:
        values = values.astype(jnp.float32).reshape(size * capp, width).astype(jnp.bfloat16)
    else:
        values = values.reshape(size * capp, width)
    acc[...] += jnp.dot(high, values, preferred_element_type=jnp.float32) + jnp.dot(
        low, values, preferred_element_type=jnp.float32
    )
    out[...] = acc[...].astype(jnp.bfloat16)

    def finish(step, carry):
        @pl.when(step >= 1)
        def _():
            dispatch(step).wait_send()
            give_back(step).wait_send()

        across_line(step).wait_send()
        across_core(step).wait_send()
        core_sum(step).wait_send()
        line_sum(step).wait_send()
        return carry

    lax.fori_loop(0, size, finish, 0)


def on_device(
    pool_input,
    documents,
    group_weight,
    pool_scale,
    pool_gain,
    out_weight,
    residual,
    routing,
    route_weights,
    ffn_gain,
    expert_gate,
    expert_up,
    expert_down,
):
    size = lax.axis_size("sp")
    tokens, width = residual.shape
    channels = pool_input.shape[1]
    gate, up, down = expert_gate[0], expert_up[0], expert_down[0]
    capacity = (3 * tokens + size - 1) // size
    padded = (capacity + 7) // 8 * 8
    vmem = pl.BlockSpec(memory_space=pltpu.VMEM)
    hbm = pl.BlockSpec(memory_space=pl.ANY)
    block = (padded, width)
    return pl.pallas_call(
        functools.partial(moe_kernel, size, capacity),
        out_shape=jax.ShapeDtypeStruct((tokens, width), jnp.bfloat16),
        in_specs=[vmem] * 10 + [hbm] * 3,
        out_specs=vmem,
        scratch_shapes=[
            pltpu.VMEM(gate.shape, jnp.bfloat16),
            pltpu.VMEM(up.shape, jnp.bfloat16),
            pltpu.VMEM(down.shape, jnp.bfloat16),
            pltpu.VMEM((4 * padded, down.shape[0]), jnp.bfloat16),
            pltpu.VMEM((size,) + block, jnp.bfloat16),
            pltpu.VMEM((size, 4) + block, jnp.bfloat16),
            pltpu.VMEM((size, 4) + block, jnp.bfloat16),
            pltpu.VMEM((size, 2) + block, jnp.bfloat16),
            pltpu.VMEM((size,) + block, jnp.bfloat16),
            pltpu.VMEM((size,) + block, jnp.bfloat16),
            pltpu.VMEM((tokens, width), jnp.float32),
            pltpu.VMEM((tokens, width), jnp.bfloat16),
            pltpu.VMEM((2, tokens), jnp.float32),
            pltpu.VMEM((2, tokens, tokens), jnp.float32),
            pltpu.VMEM((2, tokens, tokens), jnp.float32),
            pltpu.VMEM((tokens, channels), jnp.bfloat16),
            pltpu.VMEM((1, tokens), jnp.int32),
            pltpu.VMEM((4, tokens, channels), jnp.bfloat16),
            pltpu.VMEM((4, 8, tokens), jnp.float32),
            pltpu.VMEM((4, tokens, channels), jnp.bfloat16),
            pltpu.VMEM((4, 8, tokens), jnp.float32),
            pltpu.VMEM((4, channels, width), jnp.bfloat16),
            pltpu.SemaphoreType.DMA((3,)),
        ]
        + [pltpu.SemaphoreType.DMA((size,))] * 12
        + [pltpu.SemaphoreType.DMA((2,))] * 2
        + [pltpu.SemaphoreType.DMA((11,))] * 2
        + [pltpu.SemaphoreType.DMA((4,))] * 4,
        compiler_params=pltpu.CompilerParams(
            collective_id=0, has_side_effects=True, vmem_limit_bytes=62 * 1024 * 1024
        ),
    )(
        pool_input,
        documents.reshape(1, -1),
        group_weight,
        pool_scale.reshape(1, -1),
        pool_gain.reshape(1, -1),
        out_weight,
        residual,
        routing.T,
        route_weights.T,
        ffn_gain.reshape(1, -1),
        gate,
        up,
        down,
    )


def solution(mesh):
    return jax.shard_map(
        on_device,
        mesh=mesh,
        in_specs=(
            P("sp", "tp"),
            P("sp"),
            P("tp", None, None),
            P("tp"),
            P("tp"),
            P("tp", None),
            P(("sp", "tp"), None),
            P(("sp", "tp"), None),
            P(("sp", "tp"), None),
            P(),
            P("sp", None, "tp"),
            P("sp", None, "tp"),
            P("sp", "tp", None),
        ),
        out_specs=P(("sp", "tp"), None),
        check_vma=False,
    )
```
